32 devices in a mesh: ep: 32 (over z, y, x, core).
Axes of the slice: x: 2, y: 2, z: 4, core: 2. Of those that a mesh axis runs over, the one named last changes fastest.
Arguments:
- tokens: bfloat16 [128, 2048], P('ep'), may hold values from -6 to 6
- lengths: int32 [128], P('ep'), may hold values from 1 to 1023
- cache_keys: bfloat16 [128, 1024, 2, 128], P('ep')
- cache_values: bfloat16 [128, 1024, 2, 128], P('ep'), may hold values from -6 to 6
- query_w: bfloat16 [2048, 1024], replicated, may hold values from -0.125 to 0.125
- key_w: bfloat16 [2048, 256], replicated, may hold values from -0.125 to 0.125
- value_w: bfloat16 [2048, 256], replicated, may hold values from -0.125 to 0.125
- out_w: bfloat16 [1024, 2048], replicated, may hold values from -0.1875 to 0.1875
- mix_lambda: float32 [8], replicated, may hold values from 0.3 to 0.8
- head_gain: float32 [128], replicated, may hold values from 0.1 to 1.9
- attn_gain: float32 [2048], replicated, may hold values from 0.1 to 1.9
- ffn_gain: float32 [2048], replicated, may hold values from 0.1 to 1.9
- routes: int32 [128, 2], P('ep'), may hold values from 0 to 1, all different within a row; in each aligned block of 4 rows (0 to 3, 4 to 7, ...) at most 4 rows name the same one
- route_weights: float32 [128, 2], P('ep'), may hold values from 0.2 to 1
- exp_gate: bfloat16 [2048, 12288], P(None, 'ep'), may hold values from -0.125 to 0.125
- exp_up: bfloat16 [2048, 12288], P(None, 'ep'), may hold values from -0.125 to 0.125
- exp_down: bfloat16 [12288, 2048], P('ep'), may hold values from -0.078125 to 0.078125
- dense_gate: bfloat16 [32, 1024, 352], P('ep'), may hold values from -0.125 to 0.125
- dense_up: bfloat16 [32, 1024, 352], P('ep'), may hold values from -0.125 to 0.125
- dense_down: bfloat16 [32, 352, 1024], P('ep'), may hold values from -0.078125 to 0.078125
- branch_gate: bfloat16 [2048], replicated, may hold values from -0.125 to 0.125
Outputs:
- output: bfloat16 [128, 2048], P('ep')
- new_keys: bfloat16 [128, 256], P('ep')
- new_values: bfloat16 [128, 256], P('ep')
The draws below stay inside these ranges and needn't reach their ends.
Inputs may be any that keep to these rules, and one draw needn't show every extreme that they name: `routes`: each row names 2 different experts; among the 4 rows of one device no expert is named by more than 4 rows, a bound that some block reaches.
All inputs are finite; a program needn't handle non-finite values.
Results may differ from the reference program's by a relative error of at most 0.015.
Values may be sent and summed in bfloat16 or wider, within the bound.
A program may use at most 128 MiB of HBM per device.

```python
import math
import jax
import jax.numpy as jnp
import numpy as np
from jax import lax

D = 2048
HEADS = 8
KV_HEADS = 2
HEAD_DIM = 128
CACHE = 1024
SEQ_DEV = 4
TOP_K = 2
SPLIT = 16
EXP_FF = 6144
DENSE_FF = 5632
EXPERTS = 2
BLOCKS = 2
CAP = 4
TOKENS = 128
N_EP = 32


def draw_cache_keys(key, part):
    shape = (TOKENS, CACHE, KV_HEADS, HEAD_DIM)
    base_key = jax.random.fold_in(jax.random.fold_in(key, 11), 0)
    values = jax.random.normal(base_key, shape, jnp.float32) * 1.75
    values = jnp.clip(values, -10.0, 10.0)
    return values.astype(jnp.bfloat16)


def plant(drawn, stream_key, least, high):
    longest = drawn.shape.index(max(drawn.shape))
    spots = []
    for shift in (0, 1):
        where = [jax.random.randint(jax.random.fold_in(stream_key, axis), (), 0, length) for axis, length in enumerate(drawn.shape)]
        where[longest] = (where[longest] + shift) % drawn.shape[longest]
        spots.append(tuple(where))
    return drawn.at[spots[0]].set(least).at[spots[1]].set(high)


def level_of(key, extent, cuts, low, top_value):
    level = 1.0
    for position, blocks in cuts:
        steps = jax.random.uniform(jax.random.fold_in(jax.random.fold_in(key, 6), position), (blocks,), jnp.float32, low / len(cuts), top_value / len(cuts))
        level = level * jnp.repeat(jnp.exp(steps), extent[position] // blocks).reshape((-1,) + (1,) * (len(extent) - 1 - position))
    return level


def deal_out(own_key, own, number, rows, number_of, top, most, lean):
    ranking = jax.random.permutation(own_key, number_of)
    packed, ordinary = load_shares(number_of, rows * top, most, lean, True), load_shares(number_of, rows * top, most, lean, False)
    places = jnp.arange(number_of)

    def named(sizes, offset_by):
        used = int((sizes > 0).sum())
        fixed = max(1, used // 4)
        passed = fixed + (places - fixed + offset_by * (used - fixed)) % max(1, number_of - fixed)
        return jnp.zeros((number_of,), jnp.int32).at[ranking[jnp.where(places < fixed, places, passed)]].set(jnp.asarray(sizes, jnp.int32))

    sizes = jnp.where(number % 4 == 0, named(packed, number // 4), named(ordinary, number - number // 4 - 1))
    mixed = jax.random.permutation(jax.random.fold_in(own, 3), number_of)
    source_of, receiver = mixed[0:number_of // 2 * 2:2], mixed[1:number_of // 2 * 2:2]
    slack = jnp.minimum(sizes[source_of] - 1, most - sizes[receiver]) // 2
    slack = jnp.where((source_of == ranking[0]) | (receiver == ranking[0]) | (sizes[receiver] == 0), 0, jnp.maximum(slack, 0))
    passed = jax.random.randint(jax.random.fold_in(own, 4), (number_of // 2,), 0, 1 << 20) % (slack + 1)
    sizes = sizes.at[source_of].add(-passed).at[receiver].add(passed)
    members = jnp.searchsorted(jnp.cumsum(sizes), jnp.arange(rows * top), side="right").astype(jnp.int32)
    listing = members.reshape(top, rows).T
    listing = listing[jax.random.permutation(jax.random.fold_in(own, 1), rows)]
    offset_by = jax.random.randint(jax.random.fold_in(own, 2), (rows, 1), 0, top)
    return jnp.take_along_axis(listing, (jnp.arange(top)[None, :] + offset_by) % top, axis=1)


def load_shares(count, total, limit, skew, full):
    loads = [(1 << 20) // math.isqrt(grade ** skew) + 1 for grade in range(1, count + 1)]
    largest = limit if full else min(limit, max(-(-total // count), total * loads[0] // sum(loads)))
    least = 1 if total - largest >= count - 1 else 0
    counts, spare = [largest] + [least] * (count - 1), total - largest - least * (count - 1)
    while spare > 0:
        free = [i for i in range(1, count) if counts[i] < largest] or [i for i in range(1, count) if counts[i] < limit]
        mass, left = sum([loads[i] for i in free]), spare
        for i in free:
            extra = min(limit - counts[i], max(1, left * loads[i] // mass), spare)
            counts[i] = counts[i] + extra
            spare = spare - extra
    return np.array(counts)


def centred(key, extent, spread, most, shards=(), kind=jnp.bfloat16):
    values = jax.random.normal(key, extent, jnp.float32) * spread
    if len(shards) > 0:
        values = level_of(key, extent, shards, -0.22, 0.18) * values
    return jnp.clip(values, min=-most, max=most).astype(kind)


def setup_inputs(seed: int = 0) -> dict:
    seeds = jax.random.split(jax.random.key(seed), 22)
    tokens = centred(seeds[0], (TOKENS, D), 1.0, 6.0, ((0, 32),))
    lengths = plant(jax.random.randint(seeds[1], (TOKENS,), 1, CACHE), jax.random.fold_in(seeds[1], 1), 1, CACHE - 1).astype(jnp.int32)
    cache_keys = draw_cache_keys(jax.random.fold_in(seeds[21], 71), 0)
    cache_values = centred(seeds[3], (TOKENS, CACHE, KV_HEADS, HEAD_DIM), 1.0, 6.0, ((0, 32),))
    query_w = centred(seeds[4], (D, HEADS * HEAD_DIM), D ** -0.5, 0.125)
    key_w = centred(seeds[5], (D, KV_HEADS * HEAD_DIM), D ** -0.5, 0.125)
    value_w = centred(seeds[6], (D, KV_HEADS * HEAD_DIM), D ** -0.5, 0.125)
    out_w = centred(seeds[7], (HEADS * HEAD_DIM, D), (HEADS * HEAD_DIM) ** -0.5, 0.1875)
    mix_lambda = jnp.clip(jax.random.uniform(seeds[8], (HEADS,), jnp.float32, 0.3, 0.8), 0.3, 0.8)
    head_gain = jnp.clip(1.0 + 0.18 * jax.random.normal(seeds[9], (HEAD_DIM,), jnp.float32), 0.1, 1.9)
    attn_gain = jnp.clip(1.0 + 0.18 * jax.random.normal(seeds[10], (D,), jnp.float32), 0.1, 1.9)
    ffn_gain = jnp.clip(1.0 + 0.18 * jax.random.normal(seeds[11], (D,), jnp.float32), 0.1, 1.9)
    routes_keys = jax.random.split(jax.random.fold_in(seeds[12], 1), TOKENS // SEQ_DEV)
    routes_turns = jax.random.permutation(jax.random.fold_in(seeds[12], 3), TOKENS // SEQ_DEV)
    routes = jax.vmap(lambda own, number: deal_out(jax.random.fold_in(seeds[12], 2), own, number, SEQ_DEV, EXPERTS, TOP_K, CAP, 1))(routes_keys, routes_turns).reshape((TOKENS, TOP_K))
    route_weights = jnp.clip(0.2 + 0.8 * jax.random.uniform(seeds[13], (TOKENS, TOP_K), jnp.float32) ** level_of(seeds[13], (TOKENS, TOP_K), ((0, 32),), -0.2, 0.2), 0.2, 1.0)
    exp_gate = centred(seeds[14], (D, EXPERTS * EXP_FF), D ** -0.5, 0.125, ((1, 32),))
    exp_up = centred(seeds[15], (D, EXPERTS * EXP_FF), D ** -0.5, 0.125, ((1, 32),))
    exp_down = centred(seeds[16], (EXPERTS * EXP_FF, D), EXP_FF ** -0.5, 0.078125, ((0, 32),))
    dense_gate = centred(seeds[17], (N_EP, D // BLOCKS, DENSE_FF // SPLIT), D ** -0.5, 0.125, ((0, 32),))
    dense_up = centred(seeds[18], (N_EP, D // BLOCKS, DENSE_FF // SPLIT), D ** -0.5, 0.125, ((0, 32),))
    dense_down = centred(seeds[19], (N_EP, DENSE_FF // SPLIT, D // BLOCKS), DENSE_FF ** -0.5, 0.078125, ((0, 32),))
    branch_gate = centred(seeds[20], (D,), D ** -0.5, 0.125)
    return {"tokens": tokens, "lengths": lengths, "cache_keys": cache_keys, "cache_values": cache_values, "query_w": query_w, "key_w": key_w, "value_w": value_w, "out_w": out_w, "mix_lambda": mix_lambda, "head_gain": head_gain, "attn_gain": attn_gain, "ffn_gain": ffn_gain, "routes": routes, "route_weights": route_weights, "exp_gate": exp_gate, "exp_up": exp_up, "exp_down": exp_down, "dense_gate": dense_gate, "dense_up": dense_up, "dense_down": dense_down, "branch_gate": branch_gate}


def rms_norm(values, gain, epsilon):
    scale = lax.rsqrt(lax.optimization_barrier(jnp.mean(values * values, axis=-1, keepdims=True)) + epsilon)
    return values * scale * gain.astype(jnp.float32)

def softmax_pair(scores, own_score, valid):
    masked = jnp.where(valid, scores, -jnp.inf)
    largest = jnp.maximum(lax.optimization_barrier(jnp.max(masked, axis=-1)), own_score)
    raised = jnp.where(valid, jnp.exp(scores - largest[..., None]), 0.0)
    own_raised = jnp.exp(own_score - largest)
    total = lax.optimization_barrier(jnp.sum(raised, axis=-1)) + own_raised
    return (raised / total[..., None], own_raised / total)

def attend_block(tokens, lengths, cache_keys, cache_values, query_w, key_w, value_w, out_w, mix_lambda, head_gain, attn_gain, ffn_gain):
    rows = tokens.shape[0]
    groups = HEADS // KV_HEADS
    half = HEAD_DIM // 2
    scale = (HEAD_DIM // 2) ** (-0.5)
    xfull = tokens.astype(jnp.float32)
    normed = rms_norm(xfull, attn_gain, 1e-06).astype(jnp.bfloat16)
    query = jnp.dot(normed, query_w, preferred_element_type=jnp.float32).astype(jnp.bfloat16)
    key_new = jnp.dot(normed, key_w, preferred_element_type=jnp.float32).astype(jnp.bfloat16)
    value_new = jnp.dot(normed, value_w, preferred_element_type=jnp.float32).astype(jnp.bfloat16)
    qfull = query.astype(jnp.float32).reshape(rows, KV_HEADS, groups, HEAD_DIM)
    knew = key_new.astype(jnp.float32).reshape(rows, KV_HEADS, HEAD_DIM)
    vnew = value_new.astype(jnp.float32).reshape(rows, KV_HEADS, HEAD_DIM)
    kcache = cache_keys.astype(jnp.float32)
    vcache = cache_values.astype(jnp.float32)
    valid = (jnp.arange(CACHE, dtype=jnp.int32)[None, :] < lengths[:, None])[:, None, None, :]
    first = jnp.einsum('sgqd,spgd->sgqp', qfull[..., :half], kcache[..., :half]) * scale
    first_own = jnp.einsum('sgqd,sgd->sgq', qfull[..., :half], knew[..., :half]) * scale
    second = jnp.einsum('sgqd,spgd->sgqp', qfull[..., half:], kcache[..., half:]) * scale
    second_own = jnp.einsum('sgqd,sgd->sgq', qfull[..., half:], knew[..., half:]) * scale
    prob_one, own_one = softmax_pair(first, first_own, valid)
    prob_two, own_two = softmax_pair(second, second_own, valid)
    lam = mix_lambda.astype(jnp.float32).reshape(KV_HEADS, groups)
    weights = (prob_one - lam[None, :, :, None] * prob_two).astype(jnp.bfloat16)
    own_weights = (own_one - lam[None] * own_two).astype(jnp.bfloat16)
    mixed = jnp.einsum('sgqp,spgd->sgqd', weights.astype(jnp.float32), vcache)
    mixed = mixed + own_weights.astype(jnp.float32)[..., None] * vnew[:, :, None, :]
    heads = rms_norm(mixed, head_gain, 1e-05).astype(jnp.bfloat16).reshape(rows, HEADS * HEAD_DIM)
    hidden_state = xfull + jnp.dot(heads, out_w, preferred_element_type=jnp.float32)
    ffn_in = rms_norm(hidden_state, ffn_gain, 1e-06).astype(jnp.bfloat16)
    return (hidden_state, ffn_in, key_new, value_new)

def reference(tokens, lengths, cache_keys, cache_values, query_w, key_w, value_w, out_w, mix_lambda, head_gain, attn_gain, ffn_gain, routes, route_weights, exp_gate, exp_up, exp_down, dense_gate, dense_up, dense_down, branch_gate):
    blocks = tokens.shape[0] // SEQ_DEV

    def one_block(pieces):
        return attend_block(pieces[0], pieces[1], pieces[2], pieces[3], query_w, key_w, value_w, out_w, mix_lambda, head_gain, attn_gain, ffn_gain)
    hidden_state, ffn_in, key_new, value_new = lax.map(one_block, (tokens.reshape(blocks, SEQ_DEV, D), lengths.reshape(blocks, SEQ_DEV), cache_keys.reshape(blocks, SEQ_DEV, CACHE, KV_HEADS, HEAD_DIM), cache_values.reshape(blocks, SEQ_DEV, CACHE, KV_HEADS, HEAD_DIM)))
    hidden_state = hidden_state.reshape(TOKENS, D)
    ffn_in = ffn_in.reshape(TOKENS, D)
    key_new = key_new.reshape(TOKENS, KV_HEADS * HEAD_DIM)
    value_new = value_new.reshape(TOKENS, KV_HEADS * HEAD_DIM)
    slots = N_EP * CAP

    def one_expert(total, expert):
        match = routes == expert
        hit = jnp.any(match, axis=-1)
        weight = lax.optimization_barrier(jnp.sum(jnp.where(match, route_weights.astype(jnp.float32), 0.0), axis=-1))
        rank = jnp.cumsum(hit.astype(jnp.int32)) - 1
        select = hit[None, :] & (rank[None, :] == jnp.arange(slots, dtype=jnp.int32)[:, None])
        chosen = jnp.dot(select.astype(jnp.bfloat16), ffn_in, preferred_element_type=jnp.float32).astype(jnp.bfloat16)
        start = (expert * EXP_FF).astype(jnp.int32)
        w_gate = lax.dynamic_slice_in_dim(exp_gate, start, EXP_FF, 1)
        w_up = lax.dynamic_slice_in_dim(exp_up, start, EXP_FF, 1)
        w_down = lax.dynamic_slice_in_dim(exp_down, start, EXP_FF, 0)
        gate_part = jnp.dot(chosen, w_gate, preferred_element_type=jnp.float32)
        up_part = jnp.dot(chosen, w_up, preferred_element_type=jnp.float32)
        act = (jax.nn.silu(gate_part) * up_part).astype(jnp.bfloat16)
        result = jnp.dot(act, w_down, preferred_element_type=jnp.float32)
        back = jnp.dot(select.astype(jnp.float32).T, result, precision=lax.Precision.HIGHEST)
        return (total + weight[:, None] * back, None)
    routed, unused = lax.scan(one_expert, jnp.zeros((TOKENS, D), jnp.float32), jnp.arange(EXPERTS, dtype=jnp.int32))
    row_span = D // BLOCKS
    col_span = DENSE_FF // SPLIT
    gate_full = dense_gate.reshape(BLOCKS, SPLIT, row_span, col_span).transpose(0, 2, 1, 3).reshape(D, DENSE_FF)
    up_full = dense_up.reshape(BLOCKS, SPLIT, row_span, col_span).transpose(0, 2, 1, 3).reshape(D, DENSE_FF)
    down_full = dense_down.reshape(BLOCKS, SPLIT, col_span, row_span).transpose(1, 2, 0, 3).reshape(DENSE_FF, D)
    gate_part = jnp.dot(ffn_in, gate_full, preferred_element_type=jnp.float32)
    up_part = jnp.dot(ffn_in, up_full, preferred_element_type=jnp.float32)
    dense_act = (jax.nn.silu(gate_part) * up_part).astype(jnp.bfloat16)
    dense = jnp.dot(dense_act, down_full, preferred_element_type=jnp.float32)
    gate = jax.nn.sigmoid(jnp.dot(ffn_in, branch_gate, preferred_element_type=jnp.float32))
    output = (hidden_state + routed + gate[:, None] * dense).astype(jnp.bfloat16)
    return (output, key_new, value_new)
```

```python
import functools

import jax
import jax.numpy as jnp
from jax import lax
from jax.experimental import pallas as pl
from jax.experimental.pallas import tpu as pltpu
from jax.sharding import PartitionSpec as P

HEADS = 8
KV_HEADS = 2
HEAD_DIM = 128
SPLIT = 16
SIDE = 128
QKV_CHUNKS = 4
ROW_CHUNK = 128

F32 = jnp.float32
BF16 = jnp.bfloat16
MESH = pl.DeviceIdType.MESH


def attention_part(
    experts,
    small,
    keys,
    values,
    query_w,
    key_w,
    value_w,
    out_w,
    ext,
    hidden,
    new_keys,
    new_values,
    kbuf,
    vbuf,
    qbuf,
    kwbuf,
    vwbuf,
    obuf,
    qscr,
    hscr,
    wsem,
    ksem,
    vsem,
    osem,
    more_loads,
    once_entered,
):
    tokens, lengths, lam, head_gain, attn_gain, ffn_gain, routes, route_weights, branch_gate = [
        dst for _, dst in small[0]
    ]
    rows, width = tokens.shape
    span = keys.shape[1]
    step = width // QKV_CHUNKS
    groups = HEADS // KV_HEADS
    half = HEAD_DIM // 2
    small_copies = [
        pltpu.make_async_copy(src, dst, small[1].at[i]) for i, (src, dst) in enumerate(small[0])
    ]
    early, late = (0, 4), (1, 2, 3, 5, 6, 7, 8)
    for i in early + late:
        small_copies[i].start()
    weight_copies = []
    for c in range(QKV_CHUNKS):
        part = pl.ds(c * step, step)
        trio = [
            pltpu.make_async_copy(src.at[part], dst.at[part], wsem.at[3 * c + i])
            for i, (src, dst) in enumerate(((query_w, qbuf), (key_w, kwbuf), (value_w, vwbuf)))
        ]
        for copy in trio:
            copy.start()
        weight_copies.append(trio)
    key_copies = [pltpu.make_async_copy(keys.at[s], kbuf.at[s], ksem.at[s]) for s in range(rows)]
    value_copies = [pltpu.make_async_copy(values.at[s], vbuf.at[s], vsem.at[s]) for s in range(rows)]
    for s in range(rows):
        key_copies[s].start()
        value_copies[s].start()
    out_copy = pltpu.make_async_copy(out_w, obuf, osem.at[0])
    out_copy.start()
    for i in early:
        small_copies[i].wait()
    once_entered()

    x = tokens[...].astype(F32)
    normed = x * lax.rsqrt(jnp.mean(x * x, axis=-1, keepdims=True) + 1e-06) * attn_gain[...]
    normed = normed.astype(BF16)
    query = jnp.zeros((rows, query_w.shape[1]), F32)
    knew = jnp.zeros((rows, key_w.shape[1]), F32)
    vnew = jnp.zeros((rows, value_w.shape[1]), F32)
    for c in range(QKV_CHUNKS):
        for copy in weight_copies[c]:
            copy.wait()
        part = slice(c * step, (c + 1) * step)
        left = normed[:, part]
        query += jnp.dot(left, qbuf[part, :], preferred_element_type=F32)
        knew += jnp.dot(left, kwbuf[part, :], preferred_element_type=F32)
        vnew += jnp.dot(left, vwbuf[part, :], preferred_element_type=F32)
    for copy in more_loads:
        copy.start()
    new_keys[...] = knew.astype(BF16)
    new_values[...] = vnew.astype(BF16)
    query = query.astype(BF16).astype(F32)
    knew = knew.astype(BF16).astype(F32)
    vnew = vnew.astype(BF16).astype(F32)
    for s in range(rows):
        for h in range(HEADS):
            qscr[s, h : h + 1, :] = query[s : s + 1, h * HEAD_DIM : (h + 1) * HEAD_DIM]

    for i in late[:3]:
        small_copies[i].wait()
    scale = half ** (-0.5)
    lane = lax.broadcasted_iota(jnp.int32, (HEADS, HEAD_DIM), 1)
    head_row = lax.broadcasted_iota(jnp.int32, (HEADS, HEAD_DIM), 0)
    col = lax.broadcasted_iota(jnp.int32, (2 * HEADS, span), 1)
    row = lax.broadcasted_iota(jnp.int32, (2 * HEADS, span), 0)
    own_group = (col % KV_HEADS) == ((row % HEADS) // groups)
    head_col = lax.broadcasted_iota(jnp.int32, (HEADS, 1), 0)
    lam_col = jnp.zeros((HEADS, 1), F32)
    for h in range(HEADS):
        lam_col = jnp.where(head_col == h, lam[h], lam_col)
    for s in range(rows):
        q = qscr[s]
        both = jnp.concatenate([jnp.where(lane < half, q, 0.0), jnp.where(lane >= half, q, 0.0)], axis=0)
        kown = jnp.zeros((HEADS, HEAD_DIM), F32)
        vown = jnp.zeros((HEADS, HEAD_DIM), F32)
        for g in range(KV_HEADS):
            mine = head_row // groups == g
            part = slice(g * HEAD_DIM, (g + 1) * HEAD_DIM)
            kown = jnp.where(mine, knew[s : s + 1, part], kown)
            vown = jnp.where(mine, vnew[s : s + 1, part], vown)
        own = jnp.sum(both * jnp.concatenate([kown, kown], axis=0), axis=-1, keepdims=True) * scale
        key_copies[s].wait()
        scores = lax.dot_general(
            both.astype(BF16), kbuf[s], (((1,), (1,)), ((), ())), preferred_element_type=F32
        ) * scale
        valid = own_group & (col < KV_HEADS * lengths[s])
        largest = jnp.maximum(
            jnp.max(jnp.where(valid, scores, -jnp.inf), axis=-1, keepdims=True), own
        )
        raised = jnp.where(valid, jnp.exp(scores - largest), 0.0)
        own_raised = jnp.exp(own - largest)
        inverse = 1.0 / (jnp.sum(raised, axis=-1, keepdims=True) + own_raised)
        prob = raised * inverse
        own_prob = own_raised * inverse
        weights = (prob[:HEADS] - lam_col * prob[HEADS:]).astype(BF16)
        own_weights = (own_prob[:HEADS] - lam_col * own_prob[HEADS:]).astype(BF16).astype(F32)
        value_copies[s].wait()
        mixed = jnp.dot(weights, vbuf[s], preferred_element_type=F32) + own_weights * vown
        normal = mixed * lax.rsqrt(jnp.mean(mixed * mixed, axis=-1, keepdims=True) + 1e-05)
        normal = normal * head_gain[...]
        for h in range(HEADS):
            hscr[s : s + 1, h * HEAD_DIM : (h + 1) * HEAD_DIM] = normal[h : h + 1, :]
    for i in late[3:]:
        small_copies[i].wait()
    out_copy.wait()
    state = x + jnp.dot(hscr[...].astype(BF16), obuf[...], preferred_element_type=F32)
    hidden[...] = state
    ffn = state * lax.rsqrt(jnp.mean(state * state, axis=-1, keepdims=True) + 1e-06)
    ffn = (ffn * ffn_gain[...]).astype(BF16)
    ext[:, :width] = ffn
    pieces = jnp.zeros((rows, SIDE), F32)
    branch = branch_gate[...].astype(F32)
    for c in range(width // SIDE):
        pieces += ffn[:, c * SIDE : (c + 1) * SIDE].astype(F32) * branch[c : c + 1, :]
    logit = jnp.sum(pieces, axis=-1, keepdims=True)
    gate = 1.0 / (1.0 + jnp.exp(-logit))
    spot = lax.broadcasted_iota(jnp.int32, (rows, SIDE), 1)
    name = spot % (SIDE // 2)
    table = jnp.where(name == experts, gate, 0.0)
    token_row = lax.broadcasted_iota(jnp.int32, (rows, SIDE), 0)
    for k in range(routes.shape[0]):
        for s in range(rows):
            here = (name == routes[k, s]) & (name < experts) & (token_row == s)
            table = table + jnp.where(here, route_weights[k, s], 0.0)
    high = table.astype(BF16).astype(F32)
    ext[:, width:] = jnp.where(spot < SIDE // 2, high, table - high).astype(BF16)


def shared_cols(cols, blocks):
    share = cols % 128 if blocks == 2 else 0
    return share if 2 * share <= cols and share % 16 == 0 else 0


def layer_kernel(
    n,
    tokens,
    lengths,
    lam,
    head_gain,
    attn_gain,
    ffn_gain,
    routes,
    route_weights,
    branch_gate,
    keys,
    values,
    query_w,
    key_w,
    value_w,
    out_w,
    exp_gate,
    exp_up,
    exp_down,
    dense_gate,
    dense_up,
    dense_down,
    out,
    new_keys,
    new_values,
    tokens_v,
    lengths_v,
    lam_v,
    head_gain_v,
    attn_gain_v,
    ffn_gain_v,
    routes_v,
    route_weights_v,
    branch_gate_v,
    small_sem,
    ext,
    hidden,
    kbuf,
    vbuf,
    qbuf,
    kwbuf,
    vwbuf,
    obuf,
    qscr,
    hscr,
    asem,
    ksem,
    vsem,
    osem,
    egbuf,
    eubuf,
    edbuf,
    dgbuf,
    dubuf,
    ddbuf,
    dswap,
    recv,
    xall,
    gpart,
    upart,
    gusend,
    gurecv,
    act,
    total,
    sib_send,
    sib_recv,
    rs_send,
    rs_recv,
    far_send,
    far_recv,
    wsem,
    ag_send_sem,
    ag_recv_sem,
    fw_send_sem,
    fw_recv_sem,
    ex_send_sem,
    ex_recv_sem,
    sib_send_sem,
    sib_recv_sem,
    rs_send_sem,
    rs_recv_sem,
    far_send_sem,
    far_recv_sem,
    swap_sem,
):
    me = lax.axis_index("ep")
    chips = n // 2
    chip, core = me // 2, lax.rem(me, 2)
    sibling = chip * 2 + 1 - core
    blocks = n // SPLIT
    experts = n // SPLIT
    rows, width = hidden.shape
    total_rows = n * rows
    chunk = min(ROW_CHUNK, total_rows)
    row_span = dense_gate.shape[2]

    def at(k):
        return lax.rem(chip + k, chips) * 2 + core

    gchips = SPLIT // 2
    block = me // SPLIT
    expert = me // SPLIT
    gchip = lax.rem(me, SPLIT) // 2
    group_rows = SPLIT * rows

    def mate(j):
        return block * SPLIT + lax.rem(gchip + j, gchips) * 2 + core

    def group(d):
        return lax.rem(block + d, blocks)

    def place(d, j):
        return group(d) * gchips + lax.rem(gchip + j, gchips)

    def source(b, j):
        home = lax.rem(block + blocks - b, blocks)
        return home * SPLIT + lax.rem(gchip + gchips - j, gchips) * 2 + core

    hidden_cols = dense_gate.shape[1]
    share = shared_cols(hidden_cols, blocks)
    rest = hidden_cols - 2 * share
    keep = share + rest
    pitch = gusend.shape[1] // 2
    if share:
        mine = pl.multiple_of(block * share, 16)
        theirs = pl.multiple_of((1 - block) * share, 16)
        in_pieces = [(theirs, 0, share), (2 * share, share, rest), (mine, keep, share), (2 * share, keep + share, rest)]
        out_pieces = [(mine, 0, share), (2 * share, share, rest)]
    else:
        in_pieces = out_pieces = [(0, 0, hidden_cols)]

    def pieces_of(src, dst, pieces):
        return [(src.at[0, pl.ds(a, size)], dst.at[pl.ds(b, size)]) for a, b, size in pieces]

    pairs = [
        pieces_of(dense_gate, dgbuf, in_pieces) + pieces_of(dense_up, dubuf, in_pieces),
        [(exp_gate, egbuf), (exp_up, eubuf)],
        [(exp_down, edbuf)],
        pieces_of(dense_down, ddbuf, out_pieces),
    ]
    load_sets = []
    for pair_set in pairs:
        first = sum(len(x) for x in load_sets)
        load_sets.append(
            [pltpu.make_async_copy(src, dst, wsem.at[first + i]) for i, (src, dst) in enumerate(pair_set)]
        )

    def wait_loads(k):
        for copy in load_sets[k]:
            copy.wait()

    barrier = pltpu.get_barrier_semaphore()

    def greet(k, carry):
        pl.semaphore_signal(barrier, inc=1, device_id=(at(k),), device_id_type=MESH)
        return carry

    lax.fori_loop(1, chips, greet, 0)
    pl.semaphore_signal(barrier, inc=1, device_id=(sibling,), device_id_type=MESH)

    swaps = []
    if share:
        swaps = [
            pltpu.make_async_remote_copy(
                src_ref=dense_down.at[0, pl.ds(theirs, share)],
                dst_ref=dswap,
                send_sem=swap_sem.at[0],
                recv_sem=swap_sem.at[1],
                device_id=(lax.rem(me + SPLIT, n),),
                device_id_type=MESH,
            )
        ]

    def once_entered():
        pl.semaphore_wait(barrier, chips)
        for copy in swaps:
            copy.start()

    small = [
        (tokens, tokens_v),
        (lengths, lengths_v),
        (lam, lam_v),
        (head_gain, head_gain_v),
        (attn_gain, attn_gain_v),
        (ffn_gain, ffn_gain_v),
        (routes, routes_v),
        (route_weights, route_weights_v),
        (branch_gate, branch_gate_v),
    ]
    attention_part(
        experts, (small, small_sem), keys, values, query_w, key_w, value_w, out_w, ext, hidden,
        new_keys, new_values, kbuf, vbuf, qbuf, kwbuf, vwbuf, obuf, qscr, hscr,
        asem, ksem, vsem, osem, sum(load_sets, []), once_entered,
    )

    def send_block(ref, owner, q, target):
        return pltpu.make_async_remote_copy(
            src_ref=ref,
            dst_ref=recv.at[owner],
            send_sem=ag_send_sem.at[q],
            recv_sem=ag_recv_sem.at[q],
            device_id=(target,),
            device_id_type=MESH,
        )

    def near_copy(j):
        return send_block(ext, me, j, mate(j))

    def far_copy(b):
        return send_block(ext, me, b * gchips, group(b) * SPLIT + lax.rem(me, SPLIT))

    def relay_copy(b, j):
        owner = source(b, 0)
        return send_block(recv.at[owner], owner, b * gchips + j, mate(j))

    def fw_copy(b, j):
        owner = source(b, j)
        return pltpu.make_async_remote_copy(
            src_ref=recv.at[owner],
            dst_ref=recv.at[owner],
            send_sem=fw_send_sem.at[b * gchips + j],
            recv_sem=fw_recv_sem.at[b * gchips + j],
            device_id=(sibling,),
            device_id_type=MESH,
        )

    own_copy = pltpu.make_async_remote_copy(
        src_ref=ext,
        dst_ref=recv.at[me],
        send_sem=fw_send_sem.at[0],
        recv_sem=fw_recv_sem.at[0],
        device_id=(sibling,),
        device_id_type=MESH,
    )

    def loop(low, high, body):
        def run(i, carry):
            body(i)
            return carry

        lax.fori_loop(low, high, run, 0)

    for b in range(1, blocks):
        far_copy(b).start()
    loop(1, gchips, lambda j: near_copy(j).start())
    own_copy.start()
    recv[me] = ext[...]
    for b in range(1, blocks):
        far_copy(b).wait_recv()
        loop(1, gchips, lambda j: relay_copy(b, j).start())
        fw_copy(b, 0).start()

    def near_forward(j):
        near_copy(j).wait_recv()
        fw_copy(0, j).start()

    loop(1, gchips, near_forward)
    own_copy.wait_recv()
    loop(1, gchips, lambda j: fw_copy(0, j).wait_recv())

    def widen(home):
        def one(i):
            c = home * gchips + i
            pair = jnp.concatenate([recv[2 * c].astype(F32), recv[2 * c + 1].astype(F32)], axis=0)
            xall[pl.ds(pl.multiple_of(c * 2 * rows, 2 * rows), 2 * rows), :] = pair

        loop(0, gchips, one)

    def group_part(d):
        return pl.ds(pl.multiple_of(group(d) * group_rows, group_rows), group_rows)

    def by_rows(body):
        if total_rows == chunk:
            body(pl.ds(0, chunk))
        else:

            def run(r, carry):
                body(pl.ds(pl.multiple_of(r * chunk, chunk), chunk))
                return carry

            lax.fori_loop(0, total_rows // chunk, run, 0)

    wait_loads(0)

    def dense_in(part):
        left = xall[part, pl.ds(pl.multiple_of(block * row_span, 128), row_span)].astype(BF16)
        across = (((1,), (1,)), ((), ()))

        def product(buf, at):
            return lax.dot_general(left, buf[at : at + keep, :], across, preferred_element_type=F32)

        g, u = product(dgbuf, 0), product(dubuf, 0)
        gusend[part, :keep] = g.astype(BF16)
        gusend[part, pitch : pitch + keep] = u.astype(BF16)
        if share:
            g, u = product(dgbuf, keep), product(dubuf, keep)
        gpart[part, :] = g
        upart[part, :] = u

    def exchange(b):
        part = group_part(b)
        copies = []
        for j in range(1, blocks):
            slot = b * (blocks - 1) + j - 1
            copies.append(
                pltpu.make_async_remote_copy(
                    src_ref=gusend.at[part],
                    dst_ref=gurecv.at[j - 1, part],
                    send_sem=ex_send_sem.at[slot],
                    recv_sem=ex_recv_sem.at[slot],
                    device_id=(lax.rem(me + j * SPLIT, n),),
                    device_id_type=MESH,
                )
            )
        for copy in copies:
            copy.start()
        return copies

    if keep < pitch:
        gusend[...] = jnp.zeros_like(gusend)
    widen(block)
    dense_in(group_part(0))
    exchanges = [exchange(0)]
    for b in range(1, blocks):

        def relay_forward(j):
            relay_copy(b, j).wait_recv()
            fw_copy(b, j).start()

        loop(1, gchips, relay_forward)
    for b in range(1, blocks):
        loop(0, gchips, lambda j: fw_copy(b, j).wait_recv())
    for b in range(1, blocks):
        widen(group(b))
        dense_in(group_part(b))
        exchanges.append(exchange(b))

    wait_loads(1)

    def expert_in(part):
        left = xall[part, :width].astype(BF16)
        g = jnp.dot(left, egbuf[...], preferred_element_type=F32)
        u = jnp.dot(left, eubuf[...], preferred_element_type=F32)
        act[part, :] = (g / (1.0 + jnp.exp(-g)) * u).astype(BF16)

    by_rows(expert_in)
    wait_loads(2)

    def side_value(part, which):
        side = xall[part, width:]
        spot = lax.broadcasted_iota(jnp.int32, side.shape, 1) % (SIDE // 2)
        return jnp.sum(jnp.where(spot == which, side, 0.0), axis=-1, keepdims=True)

    def expert_out(part):
        product = jnp.dot(act[part, :], edbuf[...], preferred_element_type=F32)
        total[part, :] = product * side_value(part, expert)

    by_rows(expert_out)
    wait_loads(3)
    for copy in swaps:
        copy.wait_recv()

    def dense_out(part):
        g = gpart[part, :]
        u = upart[part, :]
        for j in range(blocks - 1):
            g = g + gurecv[j, part, :keep].astype(F32)
            u = u + gurecv[j, part, pitch : pitch + keep].astype(F32)
        dact = (g / (1.0 + jnp.exp(-g)) * u).astype(BF16)
        product = jnp.dot(dact, ddbuf[...], preferred_element_type=F32)
        cols = pl.ds(pl.multiple_of(block * row_span, 128), row_span)
        gate = side_value(part, experts)
        total[part, cols] = total[part, cols] + product * gate
        if share:
            across = jnp.dot(dact[:, :share], dswap[...], preferred_element_type=F32)
            cols = pl.ds(pl.multiple_of((1 - block) * row_span, 128), row_span)
            total[part, cols] = total[part, cols] + across * gate

    def both_halves(d, j):
        c = place(d, j)
        pair = total[pl.ds(pl.multiple_of(c * 2 * rows, 2 * rows), 2 * rows), :]
        return pair[:rows], pair[rows:]

    def sib_copy(q):
        return pltpu.make_async_remote_copy(
            src_ref=sib_send.at[q],
            dst_ref=sib_recv.at[q],
            send_sem=sib_send_sem.at[q],
            recv_sem=sib_recv_sem.at[q],
            device_id=(sibling,),
            device_id_type=MESH,
        )

    def rs_copy(d, j):
        q = d * gchips + j
        return pltpu.make_async_remote_copy(
            src_ref=rs_send.at[q],
            dst_ref=rs_recv.at[q],
            send_sem=rs_send_sem.at[q],
            recv_sem=rs_recv_sem.at[q],
            device_id=(mate(j),),
            device_id_type=MESH,
        )

    def cross_copy(d):
        return pltpu.make_async_remote_copy(
            src_ref=far_send.at[d - 1],
            dst_ref=far_recv.at[d - 1],
            send_sem=far_send_sem.at[d - 1],
            recv_sem=far_recv_sem.at[d - 1],
            device_id=(group(d) * SPLIT + lax.rem(me, SPLIT),),
            device_id_type=MESH,
        )

    def collect(d, acc):
        def one(j, acc):
            rs_copy(d, j).wait_recv()
            return acc + rs_recv[d * gchips + j].astype(F32)

        return lax.fori_loop(1, gchips, one, acc)

    def add_sibling(d, j):
        q = d * gchips + j
        sib_copy(q).wait_recv()
        low, high = both_halves(d, j)
        return jnp.where(core == 0, low, high) + sib_recv[q].astype(F32)

    for d in list(range(1, blocks)) + [0]:
        for j in range(1, blocks):
            exchanges[(j + d) % blocks][j - 1].wait_recv()
        dense_out(group_part(d))

        def pack(j):
            low, high = both_halves(d, j)
            sib_send[d * gchips + j] = jnp.where(core == 0, high, low).astype(BF16)

        def forward(j):
            rs_send[d * gchips + j] = add_sibling(d, j).astype(BF16)
            rs_copy(d, j).start()

        loop(0, gchips, pack)
        loop(0, gchips, lambda j: sib_copy(d * gchips + j).start())
        loop(1, gchips, forward)
    for far in range(1, blocks):
        reduced = collect(far, add_sibling(far, 0))
        far_send[far - 1] = reduced.astype(BF16)
        cross_copy(far).start()
    result = collect(0, hidden[...] + add_sibling(0, 0))
    for d in range(1, blocks):
        cross_copy(d).wait_recv()
        result = result + far_recv[d - 1].astype(F32)
    out[...] = result.astype(BF16)

    for b in range(1, blocks):
        far_copy(b).wait_send()
        loop(1, gchips, lambda j: relay_copy(b, j).wait_send())
        loop(0, gchips, lambda j: fw_copy(b, j).wait_send())
        loop(1, gchips, lambda j: rs_copy(b, j).wait_send())
        cross_copy(b).wait_send()
    own_copy.wait_send()

    def drain(j):
        near_copy(j).wait_send()
        fw_copy(0, j).wait_send()
        rs_copy(0, j).wait_send()

    loop(1, gchips, drain)
    loop(0, chips, lambda q: sib_copy(q).wait_send())
    for copies in exchanges + [swaps]:
        for copy in copies:
            copy.wait_send()


def finish_kernel(count, *refs):
    sources, targets, sem = refs[:count], refs[count : 2 * count], refs[2 * count]
    copies = [pltpu.make_async_copy(sources[i], targets[i], sem.at[i]) for i in range(count)]
    for copy in copies:
        copy.start()
    for copy in copies:
        copy.wait()


def per_device(
    n,
    tokens,
    lengths,
    cache_keys,
    cache_values,
    query_w,
    key_w,
    value_w,
    out_w,
    mix_lambda,
    head_gain,
    attn_gain,
    ffn_gain,
    routes,
    route_weights,
    exp_gate,
    exp_up,
    exp_down,
    dense_gate,
    dense_up,
    dense_down,
    branch_gate,
):
    rows, width = tokens.shape
    cache_len = cache_keys.shape[1]
    span = cache_len * KV_HEADS
    experts = n // SPLIT
    vmem = pl.BlockSpec(memory_space=pltpu.VMEM)
    anywhere = pl.BlockSpec(memory_space=pl.ANY)
    all_rows = n * rows
    chips = n // 2
    cols = dense_gate.shape[2]
    share = shared_cols(cols, n // SPLIT)
    keep = cols - share
    pitch = -(-keep // 128) * 128
    in_rows = 2 * keep if share else cols
    others = max(1, n // SPLIT - 1)
    sem = pltpu.SemaphoreType.DMA
    dense_gate = jnp.swapaxes(dense_gate, 1, 2)
    dense_up = jnp.swapaxes(dense_up, 1, 2)
    routes = routes.T
    route_weights = route_weights.T
    results = pl.pallas_call(
        functools.partial(layer_kernel, n),
        name="layer",
        out_shape=(
            pltpu.VMEM((rows, width), BF16),
            pltpu.VMEM((rows, key_w.shape[1]), BF16),
            pltpu.VMEM((rows, value_w.shape[1]), BF16),
        ),
        in_specs=[anywhere] * 21,
        out_specs=(vmem,) * 3,
        scratch_shapes=[
            pltpu.VMEM((rows, width), BF16),
            pltpu.SMEM(lengths.shape, jnp.int32),
            pltpu.SMEM(mix_lambda.shape, F32),
            pltpu.VMEM((1, HEAD_DIM), F32),
            pltpu.VMEM((1, width), F32),
            pltpu.VMEM((1, width), F32),
            pltpu.SMEM(routes.shape, jnp.int32),
            pltpu.SMEM(route_weights.shape, F32),
            pltpu.VMEM((width // SIDE, SIDE), BF16),
            sem((9,)),
            pltpu.VMEM((rows, width + SIDE), BF16),
            pltpu.VMEM((rows, width), F32),
            pltpu.VMEM((rows, span, HEAD_DIM), BF16),
            pltpu.VMEM((rows, span, HEAD_DIM), BF16),
            pltpu.VMEM(query_w.shape, BF16),
            pltpu.VMEM(key_w.shape, BF16),
            pltpu.VMEM(value_w.shape, BF16),
            pltpu.VMEM(out_w.shape, BF16),
            pltpu.VMEM((rows, HEADS, HEAD_DIM), F32),
            pltpu.VMEM((rows, HEADS * HEAD_DIM), F32),
            sem((3 * QKV_CHUNKS,)),
            sem((rows,)),
            sem((rows,)),
            sem((1,)),
            pltpu.VMEM(exp_gate.shape, BF16),
            pltpu.VMEM(exp_up.shape, BF16),
            pltpu.VMEM(exp_down.shape, BF16),
            pltpu.VMEM((in_rows, dense_gate.shape[2]), BF16),
            pltpu.VMEM((in_rows, dense_up.shape[2]), BF16),
            pltpu.VMEM((keep, dense_down.shape[2]), BF16),
            pltpu.VMEM((max(share, 16), dense_down.shape[2]), BF16),
            pltpu.VMEM((n, rows, width + SIDE), BF16),
            pltpu.VMEM((all_rows, width + SIDE), F32),
            pltpu.VMEM((all_rows, keep), F32),
            pltpu.VMEM((all_rows, keep), F32),
            pltpu.VMEM((all_rows, 2 * pitch), BF16),
            pltpu.VMEM((others, all_rows, 2 * pitch), BF16),
            pltpu.VMEM((all_rows, exp_gate.shape[1]), BF16),
            pltpu.VMEM((all_rows, width), F32),
            pltpu.VMEM((chips, rows, width), BF16),
            pltpu.VMEM((chips, rows, width), BF16),
            pltpu.VMEM((chips, rows, width), BF16),
            pltpu.VMEM((chips, rows, width), BF16),
            pltpu.VMEM((others, rows, width), BF16),
            pltpu.VMEM((others, rows, width), BF16),
            sem((13,)),
            sem((chips,)),
            sem((chips,)),
            sem((chips,)),
            sem((chips,)),
            sem((others * (n // SPLIT),)),
            sem((others * (n // SPLIT),)),
            sem((chips,)),
            sem((chips,)),
            sem((chips,)),
            sem((chips,)),
            sem((others,)),
            sem((others,)),
            sem((2,)),
        ],
        compiler_params=pltpu.CompilerParams(
            collective_id=0, has_side_effects=True, vmem_limit_bytes=63 * 2**20
        ),
    )(
        tokens,
        lengths,
        mix_lambda,
        head_gain.reshape(1, HEAD_DIM),
        attn_gain.reshape(1, width),
        ffn_gain.reshape(1, width),
        routes,
        route_weights,
        branch_gate.reshape(width // SIDE, SIDE),
        cache_keys.reshape(rows, span, HEAD_DIM),
        cache_values.reshape(rows, span, HEAD_DIM),
        query_w,
        key_w,
        value_w,
        out_w,
        exp_gate,
        exp_up,
        exp_down,
        dense_gate,
        dense_up,
        dense_down,
    )
    count = len(results)
    return pl.pallas_call(
        functools.partial(finish_kernel, count),
        name="finish",
        out_shape=tuple(jax.ShapeDtypeStruct(r.shape, r.dtype) for r in results),
        in_specs=[vmem] * count,
        out_specs=(anywhere,) * count,
        scratch_shapes=[sem((count,))],
        compiler_params=pltpu.CompilerParams(vmem_limit_bytes=2**20),
    )(*results)


def solution(mesh):
    placed = (
        P("ep", None),
        P("ep"),
        P("ep", None, None, None),
        P("ep", None, None, None),
        P(),
        P(),
        P(),
        P(),
        P(),
        P(),
        P(),
        P(),
        P("ep", None),
        P("ep", None),
        P(None, "ep"),
        P(None, "ep"),
        P("ep", None),
        P("ep", None, None),
        P("ep", None, None),
        P("ep", None, None),
        P(),
    )
    return jax.shard_map(
        functools.partial(per_device, mesh.shape["ep"]),
        mesh=mesh,
        in_specs=placed,
        out_specs=(P("ep", None), P("ep", None), P("ep", None)),
        check_vma=False,
    )
```
